32 devices in a mesh: rep: 2 (over x), fs: 8 (over z, y), tp: 2 (over core).
Axes of the slice: x: 2, y: 2, z: 4, core: 2. Of those that a mesh axis runs over, the one named last changes fastest.
Arguments:
- x_late: bfloat16 [2048, 2048], P(('rep', 'fs')), parts along dimension 0, may hold values from -6 to 6
- x_early: bfloat16 [2048, 2048], P(('rep', 'fs')), parts along dimension 0, may hold values from -6 to 6
- cotangent: bfloat16 [2048, 2048], P(('rep', 'fs')), parts along dimension 0, may hold values from -6 to 6
- pre_gain: float32 [2048], replicated, may hold values from 0.1 to 1.9
- post_gain: float32 [2048], replicated, may hold values from 0.1 to 1.9
- gate_weight: bfloat16 [2048, 3072], P('fs', 'tp'), may hold values from -0.125 to 0.125
- up_weight: bfloat16 [2048, 3072], P('fs', 'tp'), may hold values from -0.125 to 0.125
- down_weight: bfloat16 [2048, 3072], P('fs', 'tp'), may hold values from -0.109375 to 0.109375
- down_grad_sum: float32 [4096, 3072], P(('rep', 'fs'), 'tp'), parts along dimension 0, may hold values from -6 to 6
Outputs:
- y_late: bfloat16 [2048, 2048], P(('rep', 'fs')), parts along dimension 0
- dx_early: bfloat16 [2048, 2048], P(('rep', 'fs')), parts along dimension 0
- down_grad_out: float32 [4096, 3072], P(('rep', 'fs'), 'tp'), parts along dimension 0
The draws below stay inside these ranges and needn't reach their ends.
There are 2 independent parts, one for each index of `rep`. The reference program is written for one: setup_inputs(seed, part) draws one part's arguments, and reference() takes and returns one part's arrays. A program takes and returns all parts, laid end to end along the dimension named above; an argument that names none is the same for every part. Nothing has to cross between parts.
All inputs are finite; a program needn't handle non-finite values.
Results may differ from the reference program's by a relative error of at most 0.023.
Values may be sent and summed in bfloat16 or wider, within the bound.
A program may use at most 64 MiB of HBM per device.

```python
import jax
import jax.numpy as jnp
from jax import lax

D = 2048
FF = 3072
TOKENS = 1024
N_TP = 2


def strengthened(array, key, source, target, blocks, factor):
    owner, partner = [(jnp.arange(array.shape[position]) // (array.shape[position] // blocks)).reshape([-1 if axis == position else 1 for axis in range(array.ndim)]) for position in (source, target)]
    chosen = jax.random.permutation(key, blocks)[partner]
    strong = (owner == chosen) | (owner == (partner + blocks // 2) % blocks)
    return jnp.where(strong, factor * array, array)


def block_scale(own_key, dims, pieces, smallest, top_value):
    def one(position, parts):
        heights = jax.random.uniform(jax.random.fold_in(jax.random.fold_in(own_key, 6), position), (parts,), jnp.float32, smallest / len(pieces), top_value / len(pieces))
        return jnp.repeat(jnp.exp(heights), dims[position] // parts).reshape((-1,) + (1,) * (len(dims) - position - 1))

    level = one(*pieces[0])
    for cut in pieces[1:]:
        level = level * one(*cut)
    return level


def noise(key, dims, scale, most, shards=(), dtype=jnp.bfloat16):
    loudness = block_scale(key, dims, shards, -0.22, 0.18) if shards else 1.0
    result = jax.random.normal(key, dims, jnp.float32) * scale * loudness
    return jnp.minimum(jnp.maximum(result, -most), most).astype(dtype)


def gaussian_with(rng, dims, spread, most, pieces, heavy, held_as=jnp.bfloat16):
    result = spread * jax.random.normal(rng, dims, jnp.float32)
    if pieces:
        result = result * block_scale(rng, dims, pieces, -0.22, 0.18)
    return jnp.clip(strengthened(result, jax.random.fold_in(rng, 3), *heavy), -most, most).astype(held_as)


def setup_inputs(seed: int = 0, part: int = 0) -> dict:
    splits = jax.random.split(jax.random.key(seed), 10)
    part_keys = jax.random.split(jax.random.fold_in(splits[9], part), 10)
    return {
        "x_late": noise(part_keys[0], (TOKENS, D), 1.0, 6.0, ((0, 8),)),
        "x_early": noise(part_keys[1], (TOKENS, D), 1.0, 6.0, ((0, 8),)),
        "cotangent": gaussian_with(part_keys[2], (TOKENS, D), 1.0, 6.0, ((0, 8),), (0, 1, 8, 2.0)),
        "pre_gain": jnp.clip(1.0 + 0.18 * jax.random.normal(splits[3], (D,), jnp.float32), 0.1, 1.9),
        "post_gain": jnp.clip(1.0 + 0.18 * jax.random.normal(splits[4], (D,), jnp.float32), 0.1, 1.9),
        "gate_weight": noise(splits[5], (D, FF), D ** -0.5, 0.125, ((0, 8), (1, 2))),
        "up_weight": noise(splits[6], (D, FF), D ** -0.5, 0.125, ((0, 8), (1, 2))),
        "down_weight": noise(splits[7], (D, FF), FF ** -0.5, 0.109375, ((0, 8), (1, 2))),
        "down_grad_sum": noise(part_keys[8], (D, FF), 1.0, 6.0, ((0, 8), (1, 2)), jnp.float32),
    }


eps = 1e-06

def pre_norm(x, pre_gain):
    xf = x.astype(jnp.float32)
    scale = lax.rsqrt(lax.optimization_barrier(jnp.mean(xf * xf, axis=-1, keepdims=True)) + eps)
    return (xf, scale, (xf * scale * pre_gain).astype(jnp.bfloat16))

def block_sum(left, right, width):
    total = jnp.zeros((left.shape[0], right.shape[0]), jnp.float32)
    for block in range(N_TP):
        lo = block * width
        term = lax.dot_general(left[:, lo:lo + width], right[:, lo:lo + width], (((1,), (1,)), ((), ())), preferred_element_type=jnp.float32)
        term = lax.optimization_barrier(term.astype(jnp.bfloat16))
        total = total + term.astype(jnp.float32)
    return total

def forward_branch(normed, gate_weight, up_weight, down_weight):
    gate = jnp.dot(normed, gate_weight, preferred_element_type=jnp.float32)
    up = jnp.dot(normed, up_weight, preferred_element_type=jnp.float32)
    hidden = (jax.nn.silu(gate) * up).astype(jnp.bfloat16)
    branch = block_sum(hidden, down_weight, FF // N_TP)
    return (gate, up, hidden, branch)

def reference(x_late, x_early, cotangent, pre_gain, post_gain, gate_weight, up_weight, down_weight, down_grad_sum):
    width = FF // N_TP
    late_f, late_rs, late_norm = pre_norm(x_late, pre_gain)
    gate_l, up_l, hidden_l, branch_l = forward_branch(late_norm, gate_weight, up_weight, down_weight)
    late_rz = lax.rsqrt(lax.optimization_barrier(jnp.mean(branch_l * branch_l, axis=-1, keepdims=True)) + eps)
    y_late = (late_f + 0.5 * branch_l * late_rz * post_gain).astype(jnp.bfloat16)
    early_f, early_rs, early_norm = pre_norm(x_early, pre_gain)
    gate_e, up_e, hidden_e, branch_e = forward_branch(early_norm, gate_weight, up_weight, down_weight)
    early_rz = lax.rsqrt(lax.optimization_barrier(jnp.mean(branch_e * branch_e, axis=-1, keepdims=True)) + eps)
    cot_f = cotangent.astype(jnp.float32)
    dpost = 0.5 * cot_f * post_gain
    dbranch = early_rz * (dpost - branch_e * early_rz * early_rz * lax.optimization_barrier(jnp.mean(branch_e * dpost, axis=-1, keepdims=True)))
    dbranch = dbranch.astype(jnp.bfloat16)
    dhidden = jnp.dot(dbranch, down_weight, preferred_element_type=jnp.float32)
    sig = jax.nn.sigmoid(gate_e)
    dgate = (dhidden * up_e * sig * (1.0 + gate_e * (1.0 - sig))).astype(jnp.bfloat16)
    dup = (dhidden * gate_e * sig).astype(jnp.bfloat16)
    dnormed = jnp.zeros(x_early.shape, jnp.float32)
    for block in range(N_TP):
        lo = block * width
        term = lax.dot_general(dgate[:, lo:lo + width], gate_weight[:, lo:lo + width], (((1,), (1,)), ((), ())), preferred_element_type=jnp.float32)
        term = term + lax.dot_general(dup[:, lo:lo + width], up_weight[:, lo:lo + width], (((1,), (1,)), ((), ())), preferred_element_type=jnp.float32)
        term = lax.optimization_barrier(term.astype(jnp.bfloat16))
        dnormed = dnormed + term.astype(jnp.float32)
    gained = pre_gain * dnormed
    dx_early = cot_f + early_rs * (gained - early_f * early_rs * early_rs * lax.optimization_barrier(jnp.mean(early_f * gained, axis=-1, keepdims=True)))
    dx_early = dx_early.astype(jnp.bfloat16)
    down_grad_out = down_grad_sum + lax.dot_general(dbranch, hidden_e, (((0,), (0,)), ((), ())), preferred_element_type=jnp.float32)
    return (y_late, dx_early, down_grad_out)
```

```python
import functools
import itertools

import jax
import jax.numpy as jnp
from jax import lax
from jax.experimental import pallas as pl
from jax.experimental.pallas import tpu as pltpu
from jax.sharding import PartitionSpec as P

eps = 1e-06
F32, BF16 = jnp.float32, jnp.bfloat16
VMEM = pl.BlockSpec(memory_space=pltpu.VMEM)
DMA = pltpu.SemaphoreType.DMA


class Grid:
    def __init__(self, sizes):
        self.R, self.fs, self.tp = sizes
        self.fy = 2
        self.fz = self.fs // self.fy
        self.H = self.fz // 2
        self.G = self.R * self.fy
        self.offsets = list(itertools.product(range(self.R), range(self.fy)))[1:]
        self.r, self.f, self.k = (lax.axis_index(n) for n in ("rep", "fs", "tp"))
        self.h, self.y, self.b = lax.div(self.f, 4), lax.rem(lax.div(self.f, 2), 2), lax.rem(self.f, 2)
        self.z = self.h * 2 + self.b
        self.g = self.r * self.fy + self.y

    def moved(self, o, sign=1):
        dr, dy = self.offsets[o]
        r = lax.rem(self.r + self.R + sign * dr, self.R)
        y = lax.rem(self.y + self.fy + sign * dy, self.fy)
        return r, y

    def index(self, o, sign=1):
        r, y = self.moved(o, sign)
        return r * self.fy + y

    def device(self, r, z, y):
        return {"rep": r, "fs": lax.div(z, 2) * 4 + y * 2 + lax.rem(z, 2), "tp": self.k}

    def peer(self, o):
        r, y = self.moved(o)
        return self.device(r, self.z, y)

    def sibling_index(self, j):
        return lax.rem(self.k + j, self.tp)

    def sibling(self, j):
        return {"rep": self.r, "fs": self.f, "tp": self.sibling_index(j)}

    def up(self, dh):
        return lax.rem(self.h + self.H + dh, self.H)

    def along(self, dh, db):
        return self.up(dh) * 2 + lax.rem(self.b + db, 2)

    def level(self, dh, db):
        return self.device(self.r, self.along(dh, db), self.y)

    def across(self, dh, dy):
        return self.device(self.r, self.along(dh, 0), lax.rem(self.y + dy, self.fy))

    def barrier(self):
        sem = pltpu.get_barrier_semaphore()
        targets = [self.peer(o) for o in range(len(self.offsets))]
        targets += [self.sibling(j) for j in range(1, self.tp)]
        targets += [self.across(dh, dy) for dh in range(1, self.H) for dy in range(self.fy)]
        targets += [self.level(dh, 1) for dh in range(self.H)]
        for t in targets:
            pl.semaphore_signal(sem, inc=1, device_id=t, device_id_type=pl.DeviceIdType.MESH)
        pl.semaphore_wait(sem, len(targets))


class Copies:
    def __init__(self, sems):
        self.sems, self.used, self.open = sems, 0, []

    def make(self, src, dst, to, send=None, recv=None):
        if send is None:
            send = recv = self.used
            self.used += 1
        return pltpu.make_async_remote_copy(
            src_ref=src, dst_ref=dst, send_sem=self.sems.at[0, send], recv_sem=self.sems.at[1, recv],
            device_id=to, device_id_type=pl.DeviceIdType.MESH,
        )

    def push(self, src, dst, to):
        copy = self.make(src, dst, to)
        copy.start()
        return copy

    def later(self, src, dst, to):
        copy = self.push(src, dst, to)
        self.open.append(copy)
        return copy

    def finish(self):
        for copy in self.open:
            copy.wait_send()


class Weights:
    def __init__(self, m, cp, weight, wout):
        self.m, self.cp, self.weight, self.wout = m, cp, weight, wout
        self.pair, self.far, self.slot, self.over = {}, {}, {}, {}
        for i in range(3):
            for dh in range(1, m.H):
                base = cp.used
                cp.used += m.fy
                for dy in range(m.fy):
                    g = m.r * m.fy + lax.rem(m.y + dy, m.fy)
                    copy = cp.make(weight(g, i), wout.at[i, self.block(m.z, m.y)], m.across(dh, dy),
                                   base + dy, base + m.y)
                    cp.open.append(copy)
                    self.far[dh, dy, i] = copy
                self.slot[dh, i] = base

    def block(self, z, y):
        return z * self.m.fy + y

    def near(self, dh):
        return jnp.where(self.m.up(dh) > self.m.h, 1, 0) == self.m.y

    def cross(self, ii, near):
        m = self.m
        for dh in range(1, m.H):
            @pl.when(self.near(dh) == near)
            def _():
                for i in ii:
                    for dy in range(m.fy):
                        self.far[dh, dy, i].start()

    def trade(self, ii):
        m = self.m
        for i in ii:
            y = lax.rem(m.y + 1, m.fy)
            dst = self.wout.at[i, self.block(m.z, m.y)]
            self.pair[i] = self.cp.later(self.weight(m.r * m.fy + y, i), dst, m.across(0, 1))

    def pass_on(self, key, src, z, y):
        self.over[key] = self.cp.later(src, self.wout.at[key[-1], self.block(z, y)], self.m.level(0, 1))

    def own(self, ii):
        for i in ii:
            self.pass_on(("own", i), self.weight(self.m.g, i), self.m.z, self.m.y)

    def traded(self, ii):
        m = self.m
        y = lax.rem(m.y + 1, m.fy)
        for i in ii:
            self.pair[i].wait_recv()
            self.pass_on(("pair", i), self.wout.at[i, self.block(m.z, y)], m.z, y)

    def source(self, dh, near):
        m = self.m
        y = jnp.where(m.up(-dh) < m.h, 1, 0)
        return m.along(-dh, 0), y if near else 1 - y

    def crossed(self, ii, near):
        m = self.m
        for dh in range(1, m.H):
            z, y = self.source(dh, near)
            for i in ii:
                ref = self.wout.at[i, self.block(z, y)]
                base = self.slot[dh, i]
                self.cp.make(ref, ref, m.across(dh, 0), base, base + y).wait_recv()
                self.pass_on((dh, near, i), ref, z, y)

    def landed(self, key):
        self.over[key].wait_recv()

    def steps(self):
        m = self.m
        out = [("own", m.z, m.y), ("pair", m.z, lax.rem(m.y + 1, m.fy))]
        for near in (True, False):
            out += [((dh, near),) + self.source(dh, near) for dh in range(1, m.H)]
        return out


def levels(m):
    return [(dh, db) for dh in range(m.H) for db in range(2)]


class Scatter:
    def __init__(self, m, cp, p, rx, tx, rg, acc, place):
        self.m, self.cp, self.p, self.rx, self.tx, self.rg, self.acc = m, cp, p, rx, tx, rg, acc
        self.place = place
        self.pair, self.far = {}, {}

    def start(self, t):
        m = self.m
        for j in range(1, m.tp):
            src = self.p.at[t, :, :, m.sibling_index(j)]
            self.pair[t, j] = self.cp.push(src, self.rx.at[j - 1, t], m.sibling(j))

    def middle(self, t):
        m, n = self.m, len(self.m.offsets)
        for j in range(1, m.tp):
            self.pair[t, j].wait_recv()

        def total(block):
            value = self.p[t, :, block, m.k].astype(F32)
            for j in range(1, m.tp):
                value = value + self.rx[j - 1, t, :, block].astype(F32)
            return value

        for o in range(n):
            self.tx[t, o] = total(m.index(o)).astype(BF16)
            self.far[t, o] = self.cp.push(self.tx.at[t, o], self.rg.at[t, o], m.peer(o))
        self.acc[self.place(t)] = total(m.g)

    def end(self, t):
        n = len(self.m.offsets)
        for o in range(n):
            self.far[t, o].wait_recv()
        value = self.acc[self.place(t)]
        for o in range(n):
            value = value + self.rg[t, o].astype(F32)
        self.acc[self.place(t)] = value

    def finish(self):
        for copy in list(self.pair.values()) + list(self.far.values()):
            copy.wait_send()


def flat(v):
    return v.reshape(-1, v.shape[-1])


def dot(a, b, ca, cb):
    return lax.dot_general(a, b, (((ca,), (cb,)), ((), ())), preferred_element_type=F32)


def unit_scale(v):
    return lax.rsqrt(jnp.mean(v * v, axis=-1, keepdims=True) + eps)


def kernel(sizes, D, nw, *refs):
    ws, refs = refs[:nw], refs[nw:]
    (x_late, x_early, cot, pre_gain, post_gain, y_out, dx_out, owned_out,
     wout, xout, dpost, gate, up, hid, hout, p, rx, tx, rg, acc, dall, dhid, dgate, dup, dz,
           q, qx, qt, qg, dacc, dw, sems) = refs
    m = Grid(sizes)
    cp = Copies(sems)
    n, fy, tp, fz = len(m.offsets), m.fy, m.tp, m.fz
    m.barrier()
    rows, part = x_late.shape[0], wout.shape[-1]
    ce, drows = rows // tp, D // m.fs

    def weight(g, i):
        if nw == 1:
            return ws[0].at[g, i]
        return ws[i].at[:, pl.ds(pl.multiple_of(g * part, part), part)]

    def owned_at(g):
        if nw == 1:
            return owned_out.at[g]
        return owned_out.at[:, pl.ds(pl.multiple_of(g * part, part), part)]

    def columns(block):
        z, y = divmod(block, fy)
        f = (z // 2) * 4 + y * 2 + z % 2
        return slice(f * drows, (f + 1) * drows)

    both, third = (0, 1), (2,)
    w = Weights(m, cp, weight, wout)
    w.cross(both, True)
    w.trade(both)
    w.own(both)
    for t in range(tp):
        for place, ref in ((0, x_late), (ce, x_early)):
            v = ref[t * ce:(t + 1) * ce].astype(F32)
            v = (v * unit_scale(v) * pre_gain[...]).astype(BF16)
            for block in range(m.fs):
                xout[m.g, t, block, place:place + ce] = v[:, columns(block)]
    side = [o for o in range(n) if m.offsets[o][1] == 0]
    beside = m.offsets.index((0, 1))
    mine_x = xout.at[m.g, m.k]
    xz = cp.later(mine_x, mine_x, m.peer(beside))
    xs = {o: cp.later(mine_x, mine_x, m.peer(o)) for o in side}
    w.cross(both, False)
    w.cross(third, True)
    w.trade(third)
    w.cross(third, False)
    for i in range(3):
        wout[i, w.block(m.z, m.y)] = weight(m.g, i)[...]
    mine = pl.ds(pl.multiple_of(m.k * ce, ce), ce)
    v = 0.5 * cot[mine].astype(F32) * post_gain[...]
    for block in range(m.fs):
        dpost[block] = v[:, columns(block)]
    passed = []

    def share(out, g):
        for j in range(1, tp):
            passed.append(cp.push(out.at[g, m.k], out.at[g, m.k], m.sibling(j)))

    def spread(copies, out):
        for o in copies:
            copies[o].wait_recv()
            share(out, m.index(o, -1))

    w.traded(both)
    w.own(third)
    spread(xs, xout)
    w.crossed(both, True)
    xz.wait_recv()
    other = m.index(beside, -1)
    xf = {o: cp.later(xout.at[other, m.k], xout.at[other, m.k], m.peer(o)) for o in side}
    share(xout, other)
    w.crossed(third, True)
    for o in side:
        xf[o].wait_recv()
        r, _ = m.moved(o, -1)
        share(xout, r * fy + lax.rem(m.y + 1, fy))
    for copy in passed:
        copy.wait()
    passed.clear()

    gate[...] = jnp.zeros_like(gate)
    up[...] = jnp.zeros_like(up)

    def grow(block):
        def add(i, carry):
            rows = flat(xout[i, :, block])
            gate[i] += dot(rows, wout[0, block], 1, 0)
            up[i] += dot(rows, wout[1, block], 1, 0)
            return carry

        lax.fori_loop(0, m.G, add, 0)

    def twin(z):
        return lax.div(z, 2) * 2 + 1 - lax.rem(z, 2)

    steps = w.steps()
    first_far = 1 + m.H
    for s, (key, z, y) in enumerate(steps):
        key = key if isinstance(key, tuple) else (key,)
        if s == first_far:
            w.crossed(both, False)
        grow(w.block(z, y))
        for i in both:
            w.landed(key + (i,))
        grow(w.block(twin(z), y))

    def activate(i, carry):
        v = gate[i]
        hid[i] = (v * (1.0 / (1.0 + jnp.exp(-v))) * up[i]).astype(BF16)
        return carry

    lax.fori_loop(0, m.G, activate, 0)
    for t in range(tp):
        hout[m.z, t] = hid[:, (2 * t + 1) * ce:(2 * t + 2) * ce]
    w.traded(third)
    order = levels(m)
    sc = Scatter(m, cp, p, rx, tx, rg, acc, lambda t: m.along(*order[t]))
    hs, hf = {}, {}
    for t, (dh, db) in enumerate(order):
        if t == 1:
            w.landed(("own", 2))
            w.landed(("pair", 2))
        if t == 2:
            w.crossed(third, False)
            for c in range(tp):
                for d in range(1, m.H):
                    hs[d, c] = cp.later(hout.at[m.z, c], hout.at[m.z, c], m.level(d, 0))
                hf[0, c] = cp.later(hout.at[m.z, c], hout.at[m.z, c], m.level(0, 1))
        if t > 2 and db == 1:
            for near in (True, False):
                w.landed(((m.H - dh) % m.H, near, 2))
        zt = m.along(dh, db)
        for e in range(fy):
            block = zt * fy + e

            def product(i, carry, block=block, e=e):
                p[t, e, i] = dot(hid[i], wout[2, block], 1, 1).astype(BF16).reshape(p.shape[3:])
                return carry

            lax.fori_loop(0, m.G, product, 0)
        sc.start(t)
        if t:
            sc.middle(t - 1)
    sc.middle(len(order) - 1)
    for t in range(len(order)):
        sc.end(t)
    places = [divmod(block, fy) for block in range(m.fs)]

    def row_sum(term):
        return sum(jnp.sum(term(*place), axis=-1, keepdims=True) for place in places)

    rz = lax.rsqrt(row_sum(lambda t, e: acc[t, e, ce:] * acc[t, e, ce:]) / D + eps)
    mix = row_sum(lambda t, e: acc[t, e, ce:] * dpost[t * fy + e]) / D
    factor = rz * rz * mix
    for t, e in places:
        dall[m.g, m.k, t * fy + e] = (rz * (dpost[t * fy + e] - acc[t, e, ce:] * factor)).astype(BF16)
    dg = {o: cp.push(dall.at[m.g, m.k], dall.at[m.g, m.k], m.peer(o)) for o in range(n)}
    own = [cp.push(dall.at[m.g, m.k], dall.at[m.g, m.k], m.sibling(j)) for j in range(1, tp)]
    for d, c in hs:
        hs[d, c].wait_recv()
        ref = hout.at[m.along(-d, 0), c]
        hf[d, c] = cp.later(ref, ref, m.level(0, 1))
    late_rz = lax.rsqrt(row_sum(lambda t, e: acc[t, e, :ce] * acc[t, e, :ce]) / D + eps)
    for t, e in places:
        cols = columns(t * fy + e)
        v = 0.5 * acc[t, e, :ce] * late_rz * post_gain[:, cols]
        y_out[m.k, :, cols] = (x_late[mine, cols].astype(F32) + v).astype(BF16)
    spread(dg, dall)
    late = [cp.push(y_out.at[m.k], y_out.at[m.k], m.sibling(j)) for j in range(1, tp)]
    across = {}
    for s in order[1:]:
        src = dall.at[:, m.k, pl.ds(m.along(*s) * fy, fy)]
        across[s] = cp.later(src, dz.at[m.z, m.k], m.level(*s))
    for copy in passed + own:
        copy.wait()
    passed.clear()

    def back(i, carry):
        total = dot(flat(dall[i, :, 0]), wout[2, 0], 1, 0)
        for block in range(1, m.fs):
            total = total + dot(flat(dall[i, :, block]), wout[2, block], 1, 0)
        dhid[i] = total
        return carry

    lax.fori_loop(0, m.G, back, 0)

    def gates(i, carry):
        for t in range(tp):
            its, to = pl.ds((2 * t + 1) * ce, ce), pl.ds(t * ce, ce)
            g, dh = gate[i, its], dhid[i, to]
            sig = 1.0 / (1.0 + jnp.exp(-g))
            dgate[i, to] = (dh * up[i, its] * sig * (1.0 + g * (1.0 - sig))).astype(BF16)
            dup[i, to] = (dh * g * sig).astype(BF16)
        return carry

    lax.fori_loop(0, m.G, gates, 0)
    dsc = Scatter(m, cp, q, qx, qt, qg, dacc, lambda t: t)
    for t in range(fz):
        for e in range(fy):
            block = t * fy + e

            def terms(i, carry, block=block, e=e, t=t):
                v = dot(dgate[i], wout[0, block], 1, 1) + dot(dup[i], wout[1, block], 1, 1)
                q[t, e, i] = v.astype(BF16).reshape(q.shape[3:])
                return carry

            lax.fori_loop(0, m.G, terms, 0)
        dsc.start(t)
        if t:
            dsc.middle(t - 1)
    dsc.middle(fz - 1)
    for copy in hf.values():
        copy.wait_recv()
    dz[m.z] = jnp.stack([dall[:, t, pl.ds(m.z * fy, fy)] for t in range(tp)])
    for s in across:
        across[s].wait_recv()
        src = m.along(-s[0], s[1])
        for j in range(1, tp):
            passed.append(cp.push(dz.at[src, m.k], dz.at[src, m.k], m.sibling(j)))
    for t in range(fz):
        dsc.end(t)
    xf = x_early[mine].astype(F32)
    rs = unit_scale(xf)
    gained = lambda t, e: dacc[t, e] * pre_gain[:, columns(t * fy + e)]
    mix = row_sum(lambda t, e: gained(t, e) * xf[:, columns(t * fy + e)]) / D
    factor = rs * rs * mix
    for t, e in places:
        cols = columns(t * fy + e)
        v = rs * (gained(t, e) - xf[:, cols] * factor)
        dx_out[m.k, :, cols] = (cot[mine, cols].astype(F32) + v).astype(BF16)
    last = [cp.push(dx_out.at[m.k], dx_out.at[m.k], m.sibling(j)) for j in range(1, tp)]
    for copy in passed:
        copy.wait()
    sends = []

    def gradient(r, e):
        a = dz[:, :, pl.ds(r * fy, fy), e]
        b = hout[:, :, pl.ds(r * fy, fy)]
        return dot(flat(a), flat(b), 0, 0).astype(BF16)

    for o in range(n):
        r, y = m.moved(o)
        dw[o] = gradient(r, y)
        sends.append(cp.push(dw.at[o], owned_at(m.g), m.peer(o)))
    owned_at(m.g)[...] = gradient(m.r, m.y)
    for copy in sends + last + late:
        copy.wait()
    for copy in dg.values():
        copy.wait_send()
    cp.finish()
    for thing in (sc, dsc):
        thing.finish()


def body(sizes, x_late, x_early, cotangent, pre_gain, post_gain, gate_weight, up_weight, down_weight,
         down_grad_sum):
    R, fs, tp = sizes
    fy = 2
    fz, G = fs // fy, R * fy
    rows, D = x_late.shape
    drows, width = gate_weight.shape
    part = width // G
    n = G - 1
    ce = rows // tp
    c = 2 * ce
    S, V = jax.ShapeDtypeStruct, pltpu.VMEM

    weights = [gate_weight, up_weight, down_weight]
    aligned = part % 128 == 0
    if not aligned:
        weights = [jnp.stack([w.reshape(drows, G, part) for w in weights]).transpose(2, 0, 1, 3)]
    count = (3 * (2 * fz - 1) + fz * tp + 2 * (n + n * (tp - 1)) + 3 * (tp - 1)
             + 2 * fz * (tp - 1 + n) + (fz - 1) * tp + n)

    def scatter(c):
        return [
            V((fz, fy, G, tp, c, drows), BF16),
            V((tp - 1, fz, fy, G, c, drows), BF16),
            V((fz, n, fy, c, drows), BF16),
            V((fz, n, fy, c, drows), BF16),
            V((fz, fy, c, drows), F32),
        ]

    all_rows, early_rows = tp * c, tp * ce
    y_late, dx_early, owned = pl.pallas_call(
        functools.partial(kernel, sizes, D, len(weights)),
        out_shape=[
            S((tp, ce, D), BF16), S((tp, ce, D), BF16),
            S((drows, width) if aligned else (G, drows, part), BF16),
        ],
        in_specs=[VMEM] * (len(weights) + 5),
        out_specs=[VMEM] * 3,
        scratch_shapes=[
            V((3, fs, drows, part), BF16),
            V((G, tp, fs, c, drows), BF16),
            V((fs, ce, drows), F32),
            V((G, all_rows, part), F32),
            V((G, all_rows, part), F32),
            V((G, all_rows, part), BF16),
            V((fz, tp, G, ce, part), BF16),
        ] + scatter(c) + [
            V((G, tp, fs, ce, drows), BF16),
            V((G, early_rows, part), F32),
            V((G, early_rows, part), BF16),
            V((G, early_rows, part), BF16),
            V((fz, tp, G, fy, ce, drows), BF16),
        ] + scatter(ce) + [
            V((n, drows, part), BF16),
            DMA((2, count)),
        ],
        compiler_params=pltpu.CompilerParams(
            collective_id=0, has_side_effects=True, vmem_limit_bytes=60 * 1024 * 1024
        ),
    )(*weights, x_late, x_early, cotangent, pre_gain.reshape(1, D), post_gain.reshape(1, D))
    if not aligned:
        owned = owned.transpose(1, 0, 2).reshape(drows, width)
    down_grad_out = down_grad_sum + owned.astype(F32)
    return (y_late.reshape(rows, D), dx_early.reshape(rows, D), down_grad_out)


def solution(mesh):
    sizes = tuple(mesh.shape[a] for a in ("rep", "fs", "tp"))
    in_specs = (
        P(("rep", "fs"), None),
        P(("rep", "fs"), None),
        P(("rep", "fs"), None),
        P(),
        P(),
        P("fs", "tp"),
        P("fs", "tp"),
        P("fs", "tp"),
        P(("rep", "fs"), "tp"),
    )
    out_specs = (P(("rep", "fs"), None), P(("rep", "fs"), None), P(("rep", "fs"), "tp"))
    return jax.shard_map(
        functools.partial(body, sizes), mesh=mesh, in_specs=in_specs, out_specs=out_specs, check_vma=False
    )
```

```python
import functools
import itertools

import jax
import jax.numpy as jnp
from jax import lax
from jax.experimental import pallas as pl
from jax.experimental.pallas import tpu as pltpu
from jax.sharding import PartitionSpec as P

eps = 1e-06
F32, BF16 = jnp.float32, jnp.bfloat16
VMEM = pl.BlockSpec(memory_space=pltpu.VMEM)
DMA = pltpu.SemaphoreType.DMA


class Grid:
    def __init__(self, sizes):
        self.R, self.fs, self.tp = sizes
        self.fy = 2
        self.fz = self.fs // self.fy
        self.G = self.R * self.fy
        self.offsets = list(itertools.product(range(self.R), range(self.fy)))[1:]
        self.r, f, self.k = (lax.axis_index(n) for n in ("rep", "fs", "tp"))
        self.z, self.y = lax.div(f, self.fy), lax.rem(f, self.fy)
        self.g = self.r * self.fy + self.y

    def moved(self, o, sign=1):
        dr, dy = self.offsets[o]
        r = lax.rem(self.r + self.R + sign * dr, self.R)
        y = lax.rem(self.y + self.fy + sign * dy, self.fy)
        return r, y

    def index(self, o, sign=1):
        r, y = self.moved(o, sign)
        return r * self.fy + y

    def peer(self, o):
        r, y = self.moved(o)
        return {"rep": r, "fs": self.z * self.fy + y, "tp": self.k}

    def sibling_index(self, j):
        return lax.rem(self.k + j, self.tp)

    def sibling(self, j):
        return {"rep": self.r, "fs": self.z * self.fy + self.y, "tp": self.sibling_index(j)}

    def along(self, step):
        return lax.rem(self.z + self.fz + step, self.fz)

    def level(self, step):
        return {"rep": self.r, "fs": self.along(step) * self.fy + self.y, "tp": self.k}

    def barrier(self, group=False, pair=False, ring=False, levels=False):
        sem = pltpu.get_barrier_semaphore()
        targets = []
        if group:
            targets += [self.peer(o) for o in range(len(self.offsets))]
        if pair:
            targets += [self.sibling(j) for j in range(1, self.tp)]
        if levels:
            targets += [self.level(s) for s in range(1, self.fz)]
        elif ring:
            targets += [self.level(1), self.level(-1)]
        for t in targets:
            pl.semaphore_signal(sem, inc=1, device_id=t, device_id_type=pl.DeviceIdType.MESH)
        pl.semaphore_wait(sem, len(targets))


class Copies:
    def __init__(self, sems):
        self.sems, self.used = sems, 0

    def push(self, src, dst, to):
        copy = pltpu.make_async_remote_copy(
            src_ref=src, dst_ref=dst, send_sem=self.sems.at[0, self.used], recv_sem=self.sems.at[1, self.used],
            device_id=to, device_id_type=pl.DeviceIdType.MESH,
        )
        self.used += 1
        copy.start()
        return copy


class Ring:
    def __init__(self, m, cp, first, slot, chunks):
        self.m, self.cp, self.first, self.slot = m, cp, first, slot
        self.order = {0: chunks, 1: chunks[len(chunks) // 2:] + chunks[:len(chunks) // 2]}
        self.fronts = {0: set(chunks[: len(chunks) // 2]), 1: set(chunks[len(chunks) // 2:])}
        self.half = m.fz // 2
        self.sent, self.arrived = {}, set()

    def send(self, d, s, c):
        sign = 1 if d == 0 else -1
        block = self.m.along(-sign * (s - 1))
        src = self.first(c) if s == 1 else self.slot(block, c)
        self.sent[d, s, c] = self.cp.push(src, self.slot(block, c), self.m.level(sign))

    def arrive(self, d, s, c):
        if (d, s, c) not in self.sent or (d, s, c) in self.arrived:
            return
        self.sent[d, s, c].wait_recv()
        self.arrived.add((d, s, c))
        if s + 1 < self.half or (s + 1 == self.half and c in self.fronts[d]):
            self.send(d, s + 1, c)

    def step(self, s, ds=(0, 1)):
        for i in range(len(self.order[0])):
            for d in ds:
                self.arrive(d, s, self.order[d][i])

    def finish(self):
        for copy in self.sent.values():
            copy.wait_send()


def stages(m):
    half = m.fz // 2
    out = [(0, 0, ())]
    for s in range(1, half):
        out += [(-s, s, (0,)), (s, s, (1,))]
    return out + [(half, half, (0, 1))]


class Scatter:
    def __init__(self, m, cp, p, rx, tx, rg, acc, place):
        self.m, self.cp, self.p, self.rx, self.tx, self.rg, self.acc = m, cp, p, rx, tx, rg, acc
        self.place = place
        self.pair, self.hops = {}, {}
        self.side = 2 * (m.R - 1)
        self.cross = self.side + m.R
        self.back = self.cross + 1

    def start(self, t):
        m = self.m
        for j in range(1, m.tp):
            src = self.p.at[t, :, :, m.sibling_index(j)]
            self.pair[t, j] = self.cp.push(src, self.rx.at[j - 1, t], m.sibling(j))

    def total(self, t, e, dr, dy):
        m = self.m
        block = lax.rem(m.r + dr, m.R) * m.fy + lax.rem(m.y + dy, m.fy)
        value = self.p[t, e, block, m.k].astype(F32)
        for j in range(1, m.tp):
            value = value + self.rx[j - 1, t, e, block].astype(F32)
        return value

    def hop(self, t, first, count, dr, dy):
        m, part = self.m, pl.ds(first, count)
        to = m.peer(m.offsets.index((dr, dy)))
        self.hops[t, first] = self.cp.push(self.tx.at[t, part], self.rg.at[t, part], to)

    def middle(self, t):
        m = self.m
        for j in range(1, m.tp):
            self.pair[t, j].wait_recv()
        for dr in range(1, m.R):
            for dy in range(2):
                self.tx[t, 2 * (dr - 1) + dy] = self.total(t, 0, dr, dy).astype(BF16)
            self.hop(t, 2 * (dr - 1), 2, dr, 0)
        for dr in range(m.R):
            self.tx[t, self.side + dr] = self.total(t, 1, dr, 1).astype(BF16)
        self.hop(t, self.side, m.R, 0, 1)
        for e in range(2):
            self.acc[self.place(t), e] = self.total(t, e, 0, 0)

    def relay(self, t):
        m = self.m

        def got(slot):
            return self.rg[t, slot].astype(F32)

        mine, other = self.acc[self.place(t), 0], self.total(t, 0, 0, 1)
        for dr in range(1, m.R):
            self.hops[t, 2 * (dr - 1)].wait_recv()
            mine, other = mine + got(2 * (dr - 1)), other + got(2 * (dr - 1) + 1)
        self.tx[t, self.cross] = other.astype(BF16)
        self.hop(t, self.cross, 1, 0, 1)
        self.acc[self.place(t), 0] = mine
        self.hops[t, self.side].wait_recv()
        for dr in range(1, m.R):
            value = self.total(t, 1, dr, 0) + got(self.side + dr)
            self.tx[t, self.back + dr - 1] = value.astype(BF16)
            self.hop(t, self.back + dr - 1, 1, dr, 0)
        self.acc[self.place(t), 1] += got(self.side)

    def end(self, t):
        m = self.m
        self.hops[t, self.cross].wait_recv()
        self.acc[self.place(t), 0] += self.rg[t, self.cross].astype(F32)
        for dr in range(1, m.R):
            self.hops[t, self.back + dr - 1].wait_recv()
            self.acc[self.place(t), 1] += self.rg[t, self.back + dr - 1].astype(F32)

    def finish(self):
        for copy in list(self.pair.values()) + list(self.hops.values()):
            copy.wait_send()


def flat(v):
    return v.reshape(-1, v.shape[-1])


def dot(a, b, ca, cb):
    return lax.dot_general(a, b, (((ca,), (cb,)), ((), ())), preferred_element_type=F32)


def unit_scale(v):
    return lax.rsqrt(jnp.mean(v * v, axis=-1, keepdims=True) + eps)


def kernel(sizes, D, nw, *refs):
    ws, refs = refs[:nw], refs[nw:]
    (x_late, x_early, cot, pre_gain, post_gain, y_out, dx_out, owned_out,
     wout, xout, dpost, gate, up, hid, hout, p, rx, tx, rg, acc, dall, dhid, dgate, dup, dz,
           q, qx, qt, qg, dacc, dw, sems) = refs
    m = Grid(sizes)
    cp = Copies(sems)
    n, fy, tp, fz = len(m.offsets), m.fy, m.tp, m.fz
    m.barrier(group=True, pair=True, levels=True)
    f = m.z * fy + m.y
    rows, part = x_late.shape[0], wout.shape[-1]
    ce, drows = rows // tp, D // m.fs

    def weight(g, i):
        if nw == 1:
            return ws[0].at[g, i]
        return ws[i].at[:, pl.ds(pl.multiple_of(g * part, part), part)]

    def owned_at(g):
        if nw == 1:
            return owned_out.at[g]
        return owned_out.at[:, pl.ds(pl.multiple_of(g * part, part), part)]

    def columns(block):
        return slice(block * drows, (block + 1) * drows)

    def where(z, c):
        e, i = c
        return wout.at[i, z * fy + lax.rem(m.y + e, fy)]

    def first(c):
        return weight(m.g, c[1]) if c[0] == 0 else where(m.z, c)

    ys = {}

    def trade(i):
        for e in range(1, fy):
            o = m.offsets.index((0, e))
            ys[e, i] = cp.push(weight(m.index(o), i), wout.at[i, f], m.peer(o))

    ring_a = Ring(m, cp, first, where, [(e, i) for i in (0, 1) for e in range(fy)])
    ring_b = Ring(m, cp, first, where, [(e, 2) for e in range(fy)])
    trade(0)
    trade(1)
    for i in (0, 1):
        ring_a.send(0, 1, (0, i))
        ring_a.send(1, 1, (0, 1 - i))
    for t in range(tp):
        for place, ref in ((0, x_late), (ce, x_early)):
            v = ref[t * ce:(t + 1) * ce].astype(F32)
            v = (v * unit_scale(v) * pre_gain[...]).astype(BF16)
            for block in range(m.fs):
                xout[m.g, t, block, place:place + ce] = v[:, columns(block)]
    for i in range(3):
        wout[i, f] = weight(m.g, i)[...]
    xs = {o: cp.push(xout.at[m.g, m.k], xout.at[m.g, m.k], m.peer(o)) for o in range(n)}
    trade(2)
    mine = pl.ds(pl.multiple_of(m.k * ce, ce), ce)
    v = 0.5 * cot[mine].astype(F32) * post_gain[...]
    for block in range(m.fs):
        dpost[block] = v[:, columns(block)]
    for e in range(1, fy):
        back = (fy - e) % fy
        for i in (0, 1):
            ys[back, i].wait_recv()
        for i in (0, 1):
            ring_a.send(0, 1, (e, i))
            ring_a.send(1, 1, (e, 1 - i))
    for i in (0, 1):
        ring_a.arrive(0, 1, (0, i))
        ring_a.arrive(1, 1, (0, 1 - i))
    passed = []

    def spread(copies, out):
        for o in copies:
            copies[o].wait_recv()
            src = m.index(o, -1)
            for j in range(1, tp):
                passed.append(cp.push(out.at[src, m.k], out.at[src, m.k], m.sibling(j)))

    spread(xs, xout)
    ring_a.step(1)
    for e in range(fy):
        if e:
            ys[(fy - e) % fy, 2].wait_recv()
        for d in (0, 1):
            ring_b.send(d, 1, (e, 2))
    for copy in passed:
        copy.wait()
    passed.clear()

    gate[...] = jnp.zeros_like(gate)
    up[...] = jnp.zeros_like(up)
    for dist, s, ds in stages(m):
        for d in ds:
            ring_a.step(s, (d,))
        zt = m.along(dist)
        for e in range(fy):
            block = zt * fy + e

            def add(i, carry, block=block):
                rows = flat(xout[i, :, block])
                gate[i] += dot(rows, wout[0, block], 1, 0)
                up[i] += dot(rows, wout[1, block], 1, 0)
                return carry

            lax.fori_loop(0, m.G, add, 0)

    def activate(i, carry):
        v = gate[i]
        hid[i] = (v * (1.0 / (1.0 + jnp.exp(-v))) * up[i]).astype(BF16)
        return carry

    lax.fori_loop(0, m.G, activate, 0)
    for t in range(tp):
        hout[m.z, t] = hid[:, (2 * t + 1) * ce:(2 * t + 2) * ce]
    ring_h = Ring(m, cp, lambda c: hout.at[m.z, c], lambda z, c: hout.at[z, c], list(range(tp)))

    order = stages(m)
    sc = Scatter(m, cp, p, rx, tx, rg, acc, lambda t: m.along(order[t][0]))
    for t, (dist, s, ds) in enumerate(order):
        for d in ds:
            ring_b.step(s, (d,))
        if t == len(order) - 1:
            for i in range(tp):
                for d in (0, 1):
                    ring_h.send(d, 1, ring_h.order[d][i])
        zt = m.along(dist)
        for e in range(fy):
            block = zt * fy + e

            def product(i, carry, block=block, e=e):
                p[t, e, i] = dot(hid[i], wout[2, block], 1, 1).astype(BF16).reshape(p.shape[3:])
                return carry

            lax.fori_loop(0, m.G, product, 0)
        sc.start(t)
        if t:
            sc.middle(t - 1)
        if t > 1:
            sc.relay(t - 2)
    sc.middle(len(order) - 1)
    sc.relay(len(order) - 2)
    sc.relay(len(order) - 1)
    for t in range(len(order)):
        sc.end(t)
    places = [divmod(block, fy) for block in range(m.fs)]

    def row_sum(term):
        return sum(jnp.sum(term(*place), axis=-1, keepdims=True) for place in places)

    rz = lax.rsqrt(row_sum(lambda t, e: acc[t, e, ce:] * acc[t, e, ce:]) / D + eps)
    mix = row_sum(lambda t, e: acc[t, e, ce:] * dpost[t * fy + e]) / D
    factor = rz * rz * mix
    for t, e in places:
        dall[m.g, m.k, t * fy + e] = (rz * (dpost[t * fy + e] - acc[t, e, ce:] * factor)).astype(BF16)
    dg = {o: cp.push(dall.at[m.g, m.k], dall.at[m.g, m.k], m.peer(o)) for o in range(n)}
    own = [cp.push(dall.at[m.g, m.k], dall.at[m.g, m.k], m.sibling(j)) for j in range(1, tp)]
    ring_h.step(1)
    late_rz = lax.rsqrt(row_sum(lambda t, e: acc[t, e, :ce] * acc[t, e, :ce]) / D + eps)
    for t, e in places:
        cols = columns(t * fy + e)
        v = 0.5 * acc[t, e, :ce] * late_rz * post_gain[:, cols]
        y_out[m.k, :, cols] = (x_late[mine, cols].astype(F32) + v).astype(BF16)
    spread(dg, dall)
    late = [cp.push(y_out.at[m.k], y_out.at[m.k], m.sibling(j)) for j in range(1, tp)]
    across = {}
    for s in range(1, fz):
        src = dall.at[:, m.k, pl.ds(m.along(s) * fy, fy)]
        across[s] = cp.push(src, dz.at[m.z, m.k], m.level(s))
    for copy in passed + own:
        copy.wait()
    passed.clear()

    def back(i, carry):
        total = dot(flat(dall[i, :, 0]), wout[2, 0], 1, 0)
        for block in range(1, m.fs):
            total = total + dot(flat(dall[i, :, block]), wout[2, block], 1, 0)
        dhid[i] = total
        return carry

    lax.fori_loop(0, m.G, back, 0)

    def gates(i, carry):
        for t in range(tp):
            its, to = pl.ds((2 * t + 1) * ce, ce), pl.ds(t * ce, ce)
            g, dh = gate[i, its], dhid[i, to]
            sig = 1.0 / (1.0 + jnp.exp(-g))
            dgate[i, to] = (dh * up[i, its] * sig * (1.0 + g * (1.0 - sig))).astype(BF16)
            dup[i, to] = (dh * g * sig).astype(BF16)
        return carry

    lax.fori_loop(0, m.G, gates, 0)
    dsc = Scatter(m, cp, q, qx, qt, qg, dacc, lambda t: t)
    for t in range(fz):
        for e in range(fy):
            block = t * fy + e

            def terms(i, carry, block=block, e=e, t=t):
                v = dot(dgate[i], wout[0, block], 1, 1) + dot(dup[i], wout[1, block], 1, 1)
                q[t, e, i] = v.astype(BF16).reshape(q.shape[3:])
                return carry

            lax.fori_loop(0, m.G, terms, 0)
        dsc.start(t)
        if t:
            dsc.middle(t - 1)
        if t > 1:
            dsc.relay(t - 2)
    dsc.middle(fz - 1)
    dsc.relay(fz - 2)
    dsc.relay(fz - 1)
    for s in range(2, ring_h.half + 1):
        ring_h.step(s)
    dz[m.z] = jnp.stack([dall[:, t, pl.ds(m.z * fy, fy)] for t in range(tp)])
    for s in across:
        across[s].wait_recv()
        src = m.along(-s)
        for j in range(1, tp):
            passed.append(cp.push(dz.at[src, m.k], dz.at[src, m.k], m.sibling(j)))
    for copy in passed:
        copy.wait()
    sends = []

    def gradient(r, e):
        a = dz[:, :, pl.ds(r * fy, fy), e]
        b = hout[:, :, pl.ds(r * fy, fy)]
        return dot(flat(a), flat(b), 0, 0).astype(BF16)

    for o in range(n):
        r, y = m.moved(o)
        dw[o] = gradient(r, y)
        sends.append(cp.push(dw.at[o], owned_at(m.g), m.peer(o)))
    owned_at(m.g)[...] = gradient(m.r, m.y)
    for t in range(fz):
        dsc.end(t)
    xf = x_early[mine].astype(F32)
    rs = unit_scale(xf)
    gained = lambda t, e: dacc[t, e] * pre_gain[:, columns(t * fy + e)]
    mix = row_sum(lambda t, e: gained(t, e) * xf[:, columns(t * fy + e)]) / D
    factor = rs * rs * mix
    for t, e in places:
        cols = columns(t * fy + e)
        v = rs * (gained(t, e) - xf[:, cols] * factor)
        dx_out[m.k, :, cols] = (cot[mine, cols].astype(F32) + v).astype(BF16)
    last = [cp.push(dx_out.at[m.k], dx_out.at[m.k], m.sibling(j)) for j in range(1, tp)]
    for copy in sends + last + late:
        copy.wait()
    for copies in (xs, ys, dg, across):
        for copy in copies.values():
            copy.wait_send()
    for thing in (ring_a, ring_b, ring_h, sc, dsc):
        thing.finish()


def body(sizes, x_late, x_early, cotangent, pre_gain, post_gain, gate_weight, up_weight, down_weight,
         down_grad_sum):
    R, fs, tp = sizes
    fy = 2
    fz, G = fs // fy, R * fy
    rows, D = x_late.shape
    drows, width = gate_weight.shape
    part = width // G
    n = G - 1
    ce = rows // tp
    c = 2 * ce
    S, V = jax.ShapeDtypeStruct, pltpu.VMEM

    weights = [gate_weight, up_weight, down_weight]
    aligned = part % 128 == 0
    if not aligned:
        weights = [jnp.stack([w.reshape(drows, G, part) for w in weights]).transpose(2, 0, 1, 3)]
    ring = 2 * (fz // 2)
    count = (3 * (fy - 1) + ring * (3 * fy + tp) + 2 * (n + n * (tp - 1)) + 3 * (tp - 1)
             + 2 * fz * (tp - 1 + 2 * R) + (fz - 1) * tp + n)

    def scatter(c):
        return [
            V((fz, fy, G, tp, c, drows), BF16),
            V((tp - 1, fz, fy, G, c, drows), BF16),
            V((fz, 4 * R - 2, c, drows), BF16),
            V((fz, 4 * R - 2, c, drows), BF16),
            V((fz, fy, c, drows), F32),
        ]

    all_rows, early_rows = tp * c, tp * ce
    y_late, dx_early, owned = pl.pallas_call(
        functools.partial(kernel, sizes, D, len(weights)),
        out_shape=[
            S((tp, ce, D), BF16), S((tp, ce, D), BF16),
            S((drows, width) if aligned else (G, drows, part), BF16),
        ],
        in_specs=[VMEM] * (len(weights) + 5),
        out_specs=[VMEM] * 3,
        scratch_shapes=[
            V((3, fs, drows, part), BF16),
            V((G, tp, fs, c, drows), BF16),
            V((fs, ce, drows), F32),
            V((G, all_rows, part), F32),
            V((G, all_rows, part), F32),
            V((G, all_rows, part), BF16),
            V((fz, tp, G, ce, part), BF16),
        ] + scatter(c) + [
            V((G, tp, fs, ce, drows), BF16),
            V((G, early_rows, part), F32),
            V((G, early_rows, part), BF16),
            V((G, early_rows, part), BF16),
            V((fz, tp, G, fy, ce, drows), BF16),
        ] + scatter(ce) + [
            V((n, drows, part), BF16),
            DMA((2, count)),
        ],
        compiler_params=pltpu.CompilerParams(
            collective_id=0, has_side_effects=True, vmem_limit_bytes=60 * 1024 * 1024
        ),
    )(*weights, x_late, x_early, cotangent, pre_gain.reshape(1, D), post_gain.reshape(1, D))
    if not aligned:
        owned = owned.transpose(1, 0, 2).reshape(drows, width)
    down_grad_out = down_grad_sum + owned.astype(F32)
    return (y_late.reshape(rows, D), dx_early.reshape(rows, D), down_grad_out)


def solution(mesh):
    sizes = tuple(mesh.shape[a] for a in ("rep", "fs", "tp"))
    in_specs = (
        P(("rep", "fs"), None),
        P(("rep", "fs"), None),
        P(("rep", "fs"), None),
        P(),
        P(),
        P("fs", "tp"),
        P("fs", "tp"),
        P("fs", "tp"),
        P(("rep", "fs"), "tp"),
    )
    out_specs = (P(("rep", "fs"), None), P(("rep", "fs"), None), P(("rep", "fs"), "tp"))
    return jax.shard_map(
        functools.partial(body, sizes), mesh=mesh, in_specs=in_specs, out_specs=out_specs, check_vma=False
    )
```

```python
import functools
import itertools

import jax
import jax.numpy as jnp
from jax import lax
from jax.experimental import pallas as pl
from jax.experimental.pallas import tpu as pltpu
from jax.sharding import PartitionSpec as P

eps = 1e-06
F32, BF16 = jnp.float32, jnp.bfloat16
VMEM = pl.BlockSpec(memory_space=pltpu.VMEM)
DMA = pltpu.SemaphoreType.DMA


class Grid:
    def __init__(self, sizes):
        self.R, self.fs, self.tp = sizes
        self.fy = 2
        self.fz = self.fs // self.fy
        self.G = self.R * self.fy
        self.offsets = list(itertools.product(range(self.R), range(self.fy)))[1:]
        self.r, f, self.k = (lax.axis_index(n) for n in ("rep", "fs", "tp"))
        self.z, self.y = lax.div(f, self.fy), lax.rem(f, self.fy)
        self.g = self.r * self.fy + self.y

    def moved(self, o, sign=1):
        dr, dy = self.offsets[o]
        r = lax.rem(self.r + self.R + sign * dr, self.R)
        y = lax.rem(self.y + self.fy + sign * dy, self.fy)
        return r, y

    def index(self, o, sign=1):
        r, y = self.moved(o, sign)
        return r * self.fy + y

    def peer(self, o):
        r, y = self.moved(o)
        return {"rep": r, "fs": self.z * self.fy + y, "tp": self.k}

    def sibling_index(self, j):
        return lax.rem(self.k + j, self.tp)

    def sibling(self, j):
        return {"rep": self.r, "fs": self.z * self.fy + self.y, "tp": self.sibling_index(j)}

    def along(self, step):
        return lax.rem(self.z + self.fz + step, self.fz)

    def level(self, step):
        return {"rep": self.r, "fs": self.along(step) * self.fy + self.y, "tp": self.k}

    def barrier(self, group=False, pair=False, ring=False, levels=False):
        sem = pltpu.get_barrier_semaphore()
        targets = []
        if group:
            targets += [self.peer(o) for o in range(len(self.offsets))]
        if pair:
            targets += [self.sibling(j) for j in range(1, self.tp)]
        if levels:
            targets += [self.level(s) for s in range(1, self.fz)]
        elif ring:
            targets += [self.level(1), self.level(-1)]
        for t in targets:
            pl.semaphore_signal(sem, inc=1, device_id=t, device_id_type=pl.DeviceIdType.MESH)
        pl.semaphore_wait(sem, len(targets))


class Copies:
    def __init__(self, sems):
        self.sems, self.used = sems, 0

    def push(self, src, dst, to):
        copy = pltpu.make_async_remote_copy(
            src_ref=src, dst_ref=dst, send_sem=self.sems.at[0, self.used], recv_sem=self.sems.at[1, self.used],
            device_id=to, device_id_type=pl.DeviceIdType.MESH,
        )
        self.used += 1
        copy.start()
        return copy


class Ring:
    def __init__(self, m, cp, first, slot, chunks):
        self.m, self.cp, self.first, self.slot = m, cp, first, slot
        self.order = {0: chunks, 1: chunks[len(chunks) // 2:] + chunks[:len(chunks) // 2]}
        self.fronts = {0: set(chunks[: len(chunks) // 2]), 1: set(chunks[len(chunks) // 2:])}
        self.half = m.fz // 2
        self.sent, self.arrived = {}, set()

    def send(self, d, s, c):
        sign = 1 if d == 0 else -1
        block = self.m.along(-sign * (s - 1))
        src = self.first(c) if s == 1 else self.slot(block, c)
        self.sent[d, s, c] = self.cp.push(src, self.slot(block, c), self.m.level(sign))

    def arrive(self, d, s, c):
        if (d, s, c) not in self.sent or (d, s, c) in self.arrived:
            return
        self.sent[d, s, c].wait_recv()
        self.arrived.add((d, s, c))
        if s + 1 < self.half or (s + 1 == self.half and c in self.fronts[d]):
            self.send(d, s + 1, c)

    def step(self, s, ds=(0, 1)):
        for i in range(len(self.order[0])):
            for d in ds:
                self.arrive(d, s, self.order[d][i])

    def finish(self):
        for copy in self.sent.values():
            copy.wait_send()


def stages(m):
    half = m.fz // 2
    out = [(0, 0, ())]
    for s in range(1, half):
        out += [(-s, s, (0,)), (s, s, (1,))]
    return out + [(half, half, (0, 1))]


class Scatter:
    def __init__(self, m, cp, p, rx, tx, rg, acc, place, its=slice(None)):
        self.m, self.cp, self.p, self.rx, self.tx, self.rg, self.acc = m, cp, p, rx, tx, rg, acc
        self.place, self.its = place, its
        self.pair, self.hops = {}, {}
        self.side = 2 * (m.R - 1)
        self.cross = self.side + m.R
        self.back = self.cross + 1

    def start(self, t):
        m = self.m
        for j in range(1, m.tp):
            src = self.p.at[t, :, :, m.sibling_index(j), self.its]
            self.pair[t, j] = self.cp.push(src, self.rx.at[j - 1, t, :, :, self.its], m.sibling(j))

    def total(self, t, e, dr, dy):
        m = self.m
        block = lax.rem(m.r + dr, m.R) * m.fy + lax.rem(m.y + dy, m.fy)
        value = self.p[t, e, block, m.k, self.its].astype(F32)
        for j in range(1, m.tp):
            value = value + self.rx[j - 1, t, e, block, self.its].astype(F32)
        return value

    def hop(self, t, first, count, dr, dy):
        m, part = self.m, pl.ds(first, count)
        to = m.peer(m.offsets.index((dr, dy)))
        self.hops[t, first] = self.cp.push(self.tx.at[t, part, self.its], self.rg.at[t, part, self.its], to)

    def middle(self, t):
        m = self.m
        for j in range(1, m.tp):
            self.pair[t, j].wait_recv()
        for dr in range(1, m.R):
            for dy in range(2):
                self.tx[t, 2 * (dr - 1) + dy, self.its] = self.total(t, 0, dr, dy).astype(BF16)
            self.hop(t, 2 * (dr - 1), 2, dr, 0)
        for dr in range(m.R):
            self.tx[t, self.side + dr, self.its] = self.total(t, 1, dr, 1).astype(BF16)
        self.hop(t, self.side, m.R, 0, 1)
        for e in range(2):
            self.acc[self.place(t), e, self.its] = self.total(t, e, 0, 0)

    def relay(self, t):
        m = self.m

        def got(slot):
            return self.rg[t, slot, self.its].astype(F32)

        mine, other = self.acc[self.place(t), 0, self.its], self.total(t, 0, 0, 1)
        for dr in range(1, m.R):
            self.hops[t, 2 * (dr - 1)].wait_recv()
            mine, other = mine + got(2 * (dr - 1)), other + got(2 * (dr - 1) + 1)
        self.tx[t, self.cross, self.its] = other.astype(BF16)
        self.hop(t, self.cross, 1, 0, 1)
        self.acc[self.place(t), 0, self.its] = mine
        self.hops[t, self.side].wait_recv()
        for dr in range(1, m.R):
            value = self.total(t, 1, dr, 0) + got(self.side + dr)
            self.tx[t, self.back + dr - 1, self.its] = value.astype(BF16)
            self.hop(t, self.back + dr - 1, 1, dr, 0)
        self.acc[self.place(t), 1, self.its] += got(self.side)

    def end(self, t):
        m = self.m
        self.hops[t, self.cross].wait_recv()
        self.acc[self.place(t), 0, self.its] += self.rg[t, self.cross, self.its].astype(F32)
        for dr in range(1, m.R):
            self.hops[t, self.back + dr - 1].wait_recv()
            self.acc[self.place(t), 1, self.its] += self.rg[t, self.back + dr - 1, self.its].astype(F32)

    def finish(self):
        for copy in list(self.pair.values()) + list(self.hops.values()):
            copy.wait_send()


def flat(v):
    return v.reshape(-1, v.shape[-1])


def dot(a, b, ca, cb):
    return lax.dot_general(a, b, (((ca,), (cb,)), ((), ())), preferred_element_type=F32)


def unit_scale(v):
    return lax.rsqrt(jnp.mean(v * v, axis=-1, keepdims=True) + eps)


def kernel(sizes, D, nw, *refs):
    away, refs = refs[:nw], refs[nw:]
    ws, load, refs = refs[-nw - 1:-1], refs[-1], refs[:-nw - 1]
    loads = [pltpu.make_async_copy(away[i], ws[i], load.at[i]) for i in range(nw)]
    for copy in loads:
        copy.start()
    (x_late, x_early, cot, pre_gain, post_gain, y_out, dx_out, owned_out,
     wout, xout, dpost, gate, up, hid, hout, p, rx, tx, rg, acc, dall, dhid, dgate, dup, dz,
           q, qx, qt, qg, dacc, dw, sems) = refs
    m = Grid(sizes)
    cp = Copies(sems)
    n, fy, tp, fz = len(m.offsets), m.fy, m.tp, m.fz
    m.barrier(group=True, pair=True, levels=True)
    for copy in loads:
        copy.wait()
    f = m.z * fy + m.y
    rows, part = x_late.shape[0], wout.shape[-1]
    ce, drows = rows // tp, D // m.fs

    def weight(g, i):
        if nw == 1:
            return ws[0].at[g, i]
        return ws[i].at[:, pl.ds(pl.multiple_of(g * part, part), part)]

    def owned_at(g):
        if nw == 1:
            return owned_out.at[g]
        return owned_out.at[:, pl.ds(pl.multiple_of(g * part, part), part)]

    def columns(block):
        return slice(block * drows, (block + 1) * drows)

    def where(z, c):
        e, i = c
        return wout.at[i, z * fy + lax.rem(m.y + e, fy)]

    def first(c):
        return weight(m.g, c[1]) if c[0] == 0 else where(m.z, c)

    ys = {}

    def trade(i):
        for e in range(1, fy):
            o = m.offsets.index((0, e))
            ys[e, i] = cp.push(weight(m.index(o), i), wout.at[i, f], m.peer(o))

    ring_a = Ring(m, cp, first, where, [(e, i) for i in (0, 1) for e in range(fy)])
    ring_b = Ring(m, cp, first, where, [(e, 2) for e in range(fy)])
    trade(0)
    trade(1)
    for i in (0, 1):
        ring_a.send(0, 1, (0, i))
        ring_a.send(1, 1, (0, 1 - i))
    for t in range(tp):
        for place, ref in ((0, x_late), (ce, x_early)):
            v = ref[t * ce:(t + 1) * ce].astype(F32)
            v = (v * unit_scale(v) * pre_gain[...]).astype(BF16)
            for block in range(m.fs):
                xout[m.g, t, block, place:place + ce] = v[:, columns(block)]
    for i in range(3):
        wout[i, f] = weight(m.g, i)[...]
    xs = {o: cp.push(xout.at[m.g, m.k], xout.at[m.g, m.k], m.peer(o)) for o in range(n)}
    trade(2)
    mine = pl.ds(pl.multiple_of(m.k * ce, ce), ce)
    v = 0.5 * cot[mine].astype(F32) * post_gain[...]
    for block in range(m.fs):
        dpost[block] = v[:, columns(block)]
    for e in range(1, fy):
        back = (fy - e) % fy
        for i in (0, 1):
            ys[back, i].wait_recv()
        for i in (0, 1):
            ring_a.send(0, 1, (e, i))
            ring_a.send(1, 1, (e, 1 - i))
    for i in (0, 1):
        ring_a.arrive(0, 1, (0, i))
        ring_a.arrive(1, 1, (0, 1 - i))
    passed = []

    def spread(copies, out):
        for o in copies:
            copies[o].wait_recv()
            src = m.index(o, -1)
            for j in range(1, tp):
                passed.append(cp.push(out.at[src, m.k], out.at[src, m.k], m.sibling(j)))

    spread(xs, xout)
    ring_a.step(1)
    for e in range(fy):
        if e:
            ys[(fy - e) % fy, 2].wait_recv()
        for d in (0, 1):
            ring_b.send(d, 1, (e, 2))
    for copy in passed:
        copy.wait()
    passed.clear()

    gate[...] = jnp.zeros_like(gate)
    up[...] = jnp.zeros_like(up)
    for dist, s, ds in stages(m):
        for d in ds:
            ring_a.step(s, (d,))
        zt = m.along(dist)
        for e in range(fy):
            block = zt * fy + e

            def add(i, carry, block=block):
                rows = flat(xout[i, :, block])
                gate[i] += dot(rows, wout[0, block], 1, 0)
                up[i] += dot(rows, wout[1, block], 1, 0)
                return carry

            lax.fori_loop(0, m.G, add, 0)

    def activate(i, carry):
        v = gate[i]
        hid[i] = (v * (1.0 / (1.0 + jnp.exp(-v))) * up[i]).astype(BF16)
        return carry

    lax.fori_loop(0, m.G, activate, 0)
    for t in range(tp):
        hout[m.z, t] = hid[:, (2 * t + 1) * ce:(2 * t + 2) * ce]
    ring_h = Ring(m, cp, lambda c: hout.at[m.z, c], lambda z, c: hout.at[z, c], list(range(tp)))

    order = stages(m)
    halves = [pl.ds(low, ce) for low in (ce, 0)]
    sc, sl = (Scatter(m, cp, p, rx, tx, rg, acc, lambda t: m.along(order[t][0]), its) for its in halves)
    for t, (dist, s, ds) in enumerate(order):
        for d in ds:
            ring_b.step(s, (d,))
        if t == len(order) - 1:
            for i in range(tp):
                for d in (0, 1):
                    ring_h.send(d, 1, ring_h.order[d][i])
        zt = m.along(dist)
        for e in range(fy):
            block = zt * fy + e

            def product(i, carry, block=block, e=e):
                p[t, e, i] = dot(hid[i], wout[2, block], 1, 1).astype(BF16).reshape(p.shape[3:])
                return carry

            lax.fori_loop(0, m.G, product, 0)
        sc.start(t)
        sl.start(t)
        if t:
            sc.middle(t - 1)
        if t > 1:
            sc.relay(t - 2)
    sc.middle(len(order) - 1)
    sc.relay(len(order) - 2)
    sc.relay(len(order) - 1)
    for t in range(len(order)):
        sc.end(t)
    places = [divmod(block, fy) for block in range(m.fs)]

    def row_sum(term):
        return sum(jnp.sum(term(*place), axis=-1, keepdims=True) for place in places)

    rz = lax.rsqrt(row_sum(lambda t, e: acc[t, e, ce:] * acc[t, e, ce:]) / D + eps)
    mix = row_sum(lambda t, e: acc[t, e, ce:] * dpost[t * fy + e]) / D
    factor = rz * rz * mix
    for t, e in places:
        dall[m.g, m.k, t * fy + e] = (rz * (dpost[t * fy + e] - acc[t, e, ce:] * factor)).astype(BF16)
    dg = {o: cp.push(dall.at[m.g, m.k], dall.at[m.g, m.k], m.peer(o)) for o in range(n)}
    own = [cp.push(dall.at[m.g, m.k], dall.at[m.g, m.k], m.sibling(j)) for j in range(1, tp)]
    ring_h.step(1)
    for t in range(len(order)):
        sl.middle(t)
    spread(dg, dall)
    across = {}
    for s in range(1, fz):
        src = dall.at[:, m.k, pl.ds(m.along(s) * fy, fy)]
        across[s] = cp.push(src, dz.at[m.z, m.k], m.level(s))
    for copy in passed + own:
        copy.wait()
    passed.clear()

    def back(i, carry):
        total = dot(flat(dall[i, :, 0]), wout[2, 0], 1, 0)
        for block in range(1, m.fs):
            total = total + dot(flat(dall[i, :, block]), wout[2, block], 1, 0)
        dhid[i] = total
        return carry

    lax.fori_loop(0, m.G, back, 0)

    def gates(i, carry):
        for t in range(tp):
            its, to = pl.ds((2 * t + 1) * ce, ce), pl.ds(t * ce, ce)
            g, dh = gate[i, its], dhid[i, to]
            sig = 1.0 / (1.0 + jnp.exp(-g))
            dgate[i, to] = (dh * up[i, its] * sig * (1.0 + g * (1.0 - sig))).astype(BF16)
            dup[i, to] = (dh * g * sig).astype(BF16)
        return carry

    lax.fori_loop(0, m.G, gates, 0)
    for t in range(len(order)):
        sl.relay(t)
    dsc = Scatter(m, cp, q, qx, qt, qg, dacc, lambda t: t)
    for t in range(fz):
        for e in range(fy):
            block = t * fy + e

            def terms(i, carry, block=block, e=e, t=t):
                v = dot(dgate[i], wout[0, block], 1, 1) + dot(dup[i], wout[1, block], 1, 1)
                q[t, e, i] = v.astype(BF16).reshape(q.shape[3:])
                return carry

            lax.fori_loop(0, m.G, terms, 0)
        dsc.start(t)
        if t:
            dsc.middle(t - 1)
        if t > 1:
            dsc.relay(t - 2)
    dsc.middle(fz - 1)
    dsc.relay(fz - 2)
    dsc.relay(fz - 1)
    for s in range(2, ring_h.half + 1):
        ring_h.step(s)
    dz[m.z] = jnp.stack([dall[:, t, pl.ds(m.z * fy, fy)] for t in range(tp)])
    for s in across:
        across[s].wait_recv()
        src = m.along(-s)
        for j in range(1, tp):
            passed.append(cp.push(dz.at[src, m.k], dz.at[src, m.k], m.sibling(j)))
    for copy in passed:
        copy.wait()
    sends = []

    def gradient(r, e):
        a = dz[:, :, pl.ds(r * fy, fy), e]
        b = hout[:, :, pl.ds(r * fy, fy)]
        return dot(flat(a), flat(b), 0, 0).astype(BF16)

    for o in reversed(range(n)):
        r, y = m.moved(o)
        dw[o] = gradient(r, y)
        sends.append(cp.push(dw.at[o], owned_at(m.g), m.peer(o)))
    owned_at(m.g)[...] = gradient(m.r, m.y)
    for t in range(len(order)):
        sl.end(t)
    late_rz = lax.rsqrt(row_sum(lambda t, e: acc[t, e, :ce] * acc[t, e, :ce]) / D + eps)
    for t, e in places:
        cols = columns(t * fy + e)
        v = 0.5 * acc[t, e, :ce] * late_rz * post_gain[:, cols]
        y_out[m.k, :, cols] = (x_late[mine, cols].astype(F32) + v).astype(BF16)
    late = [cp.push(y_out.at[m.k], y_out.at[m.k], m.sibling(j)) for j in range(1, tp)]
    for t in range(fz):
        dsc.end(t)
    xf = x_early[mine].astype(F32)
    rs = unit_scale(xf)
    gained = lambda t, e: dacc[t, e] * pre_gain[:, columns(t * fy + e)]
    mix = row_sum(lambda t, e: gained(t, e) * xf[:, columns(t * fy + e)]) / D
    factor = rs * rs * mix
    for t, e in places:
        cols = columns(t * fy + e)
        v = rs * (gained(t, e) - xf[:, cols] * factor)
        dx_out[m.k, :, cols] = (cot[mine, cols].astype(F32) + v).astype(BF16)
    last = [cp.push(dx_out.at[m.k], dx_out.at[m.k], m.sibling(j)) for j in range(1, tp)]
    for copy in sends + last + late:
        copy.wait()
    for copies in (xs, ys, dg, across):
        for copy in copies.values():
            copy.wait_send()
    for thing in (ring_a, ring_b, ring_h, sc, sl, dsc):
        thing.finish()


def body(sizes, x_late, x_early, cotangent, pre_gain, post_gain, gate_weight, up_weight, down_weight,
         down_grad_sum):
    R, fs, tp = sizes
    fy = 2
    fz, G = fs // fy, R * fy
    rows, D = x_late.shape
    drows, width = gate_weight.shape
    part = width // G
    n = G - 1
    ce = rows // tp
    c = 2 * ce
    S, V = jax.ShapeDtypeStruct, pltpu.VMEM

    weights = [gate_weight, up_weight, down_weight]
    aligned = part % 128 == 0
    if not aligned:
        weights = [jnp.stack([w.reshape(drows, G, part) for w in weights]).transpose(2, 0, 1, 3)]
    ring = 2 * (fz // 2)
    count = (3 * (fy - 1) + ring * (3 * fy + tp) + 2 * (n + n * (tp - 1)) + 3 * (tp - 1)
             + 3 * fz * (tp - 1 + 2 * R) + (fz - 1) * tp + n)

    def scatter(c):
        return [
            V((fz, fy, G, tp, c, drows), BF16),
            V((tp - 1, fz, fy, G, c, drows), BF16),
            V((fz, 4 * R - 2, c, drows), BF16),
            V((fz, 4 * R - 2, c, drows), BF16),
            V((fz, fy, c, drows), F32),
        ]

    all_rows, early_rows = tp * c, tp * ce
    y_late, dx_early, owned = pl.pallas_call(
        functools.partial(kernel, sizes, D, len(weights)),
        out_shape=[
            S((tp, ce, D), BF16), S((tp, ce, D), BF16),
            S((drows, width) if aligned else (G, drows, part), BF16),
        ],
        in_specs=[pl.BlockSpec(memory_space=pl.ANY)] * len(weights) + [VMEM] * 5,
        out_specs=[VMEM] * 3,
        scratch_shapes=[
            V((3, fs, drows, part), BF16),
            V((G, tp, fs, c, drows), BF16),
            V((fs, ce, drows), F32),
            V((G, all_rows, part), F32),
            V((G, all_rows, part), F32),
            V((G, all_rows, part), BF16),
            V((fz, tp, G, ce, part), BF16),
        ] + scatter(c) + [
            V((G, tp, fs, ce, drows), BF16),
            V((G, early_rows, part), F32),
            V((G, early_rows, part), BF16),
            V((G, early_rows, part), BF16),
            V((fz, tp, G, fy, ce, drows), BF16),
        ] + scatter(ce) + [
            V((n, drows, part), BF16),
            DMA((2, count)),
        ] + [V(w.shape, w.dtype) for w in weights] + [DMA((len(weights),))],
        compiler_params=pltpu.CompilerParams(
            collective_id=0, has_side_effects=True, vmem_limit_bytes=60 * 1024 * 1024
        ),
    )(*weights, x_late, x_early, cotangent, pre_gain.reshape(1, D), post_gain.reshape(1, D))
    if not aligned:
        owned = owned.transpose(1, 0, 2).reshape(drows, width)
    down_grad_out = down_grad_sum + owned.astype(F32)
    return (y_late.reshape(rows, D), dx_early.reshape(rows, D), down_grad_out)


def solution(mesh):
    sizes = tuple(mesh.shape[a] for a in ("rep", "fs", "tp"))
    in_specs = (
        P(("rep", "fs"), None),
        P(("rep", "fs"), None),
        P(("rep", "fs"), None),
        P(),
        P(),
        P("fs", "tp"),
        P("fs", "tp"),
        P("fs", "tp"),
        P(("rep", "fs"), "tp"),
    )
    out_specs = (P(("rep", "fs"), None), P(("rep", "fs"), None), P(("rep", "fs"), "tp"))
    return jax.shard_map(
        functools.partial(body, sizes), mesh=mesh, in_specs=in_specs, out_specs=out_specs, check_vma=False
    )
```

```python
import functools
import itertools

import jax
import jax.numpy as jnp
from jax import lax
from jax.experimental import pallas as pl
from jax.experimental.pallas import tpu as pltpu
from jax.sharding import PartitionSpec as P

eps = 1e-06
F32, BF16 = jnp.float32, jnp.bfloat16
VMEM = pl.BlockSpec(memory_space=pltpu.VMEM)
DMA = pltpu.SemaphoreType.DMA


class Grid:
    def __init__(self, sizes):
        self.R, self.fs, self.tp = sizes
        self.fy = 2
        self.fz = self.fs // self.fy
        self.G = self.R * self.fy
        self.offsets = list(itertools.product(range(self.R), range(self.fy)))[1:]
        self.r, f, self.k = (lax.axis_index(n) for n in ("rep", "fs", "tp"))
        self.z, self.y = lax.div(f, self.fy), lax.rem(f, self.fy)
        self.g = self.r * self.fy + self.y

    def moved(self, o, sign=1):
        dr, dy = self.offsets[o]
        r = lax.rem(self.r + self.R + sign * dr, self.R)
        y = lax.rem(self.y + self.fy + sign * dy, self.fy)
        return r, y

    def index(self, o, sign=1):
        r, y = self.moved(o, sign)
        return r * self.fy + y

    def peer(self, o):
        r, y = self.moved(o)
        return {"rep": r, "fs": self.z * self.fy + y, "tp": self.k}

    def sibling_index(self, j):
        return lax.rem(self.k + j, self.tp)

    def sibling(self, j):
        return {"rep": self.r, "fs": self.z * self.fy + self.y, "tp": self.sibling_index(j)}

    def along(self, step):
        return lax.rem(self.z + self.fz + step, self.fz)

    def level(self, step):
        return {"rep": self.r, "fs": self.along(step) * self.fy + self.y, "tp": self.k}

    def barrier(self, group=False, pair=False, ring=False, levels=False):
        sem = pltpu.get_barrier_semaphore()
        targets = []
        if group:
            targets += [self.peer(o) for o in range(len(self.offsets))]
        if pair:
            targets += [self.sibling(j) for j in range(1, self.tp)]
        if levels:
            targets += [self.level(s) for s in range(1, self.fz)]
        elif ring:
            targets += [self.level(1), self.level(-1)]
        for t in targets:
            pl.semaphore_signal(sem, inc=1, device_id=t, device_id_type=pl.DeviceIdType.MESH)
        pl.semaphore_wait(sem, len(targets))


class Copies:
    def __init__(self, sems):
        self.sems, self.used = sems, 0

    def push(self, src, dst, to):
        copy = pltpu.make_async_remote_copy(
            src_ref=src, dst_ref=dst, send_sem=self.sems.at[0, self.used], recv_sem=self.sems.at[1, self.used],
            device_id=to, device_id_type=pl.DeviceIdType.MESH,
        )
        self.used += 1
        copy.start()
        return copy


class Ring:
    def __init__(self, m, cp, first, slot, chunks):
        self.m, self.cp, self.first, self.slot = m, cp, first, slot
        self.order = {0: chunks, 1: chunks[len(chunks) // 2:] + chunks[:len(chunks) // 2]}
        self.fronts = {0: set(chunks[: len(chunks) // 2]), 1: set(chunks[len(chunks) // 2:])}
        self.half = m.fz // 2
        self.sent, self.arrived = {}, set()

    def send(self, d, s, c):
        sign = 1 if d == 0 else -1
        block = self.m.along(-sign * (s - 1))
        src = self.first(c) if s == 1 else self.slot(block, c)
        self.sent[d, s, c] = self.cp.push(src, self.slot(block, c), self.m.level(sign))

    def arrive(self, d, s, c):
        if (d, s, c) not in self.sent or (d, s, c) in self.arrived:
            return
        self.sent[d, s, c].wait_recv()
        self.arrived.add((d, s, c))
        if s + 1 < self.half or (s + 1 == self.half and c in self.fronts[d]):
            self.send(d, s + 1, c)

    def step(self, s, ds=(0, 1)):
        for i in range(len(self.order[0])):
            for d in ds:
                self.arrive(d, s, self.order[d][i])

    def finish(self):
        for copy in self.sent.values():
            copy.wait_send()


def stages(m):
    half = m.fz // 2
    out = [(0, 0, ())]
    for s in range(1, half):
        out += [(-s, s, (0,)), (s, s, (1,))]
    return out + [(half, half, (0, 1))]


class Scatter:
    def __init__(self, m, cp, p, rx, tx, rg, acc, place, its=slice(None)):
        self.m, self.cp, self.p, self.rx, self.tx, self.rg, self.acc = m, cp, p, rx, tx, rg, acc
        self.place, self.its = place, its
        self.pair, self.hops = {}, {}
        self.side = 2 * (m.R - 1)
        self.cross = self.side + m.R
        self.back = self.cross + 1

    def start(self, t):
        m = self.m
        for j in range(1, m.tp):
            src = self.p.at[t, :, :, m.sibling_index(j), self.its]
            self.pair[t, j] = self.cp.push(src, self.rx.at[j - 1, t, :, :, self.its], m.sibling(j))

    def total(self, t, e, dr, dy):
        m = self.m
        block = lax.rem(m.r + dr, m.R) * m.fy + lax.rem(m.y + dy, m.fy)
        value = self.p[t, e, block, m.k, self.its].astype(F32)
        for j in range(1, m.tp):
            value = value + self.rx[j - 1, t, e, block, self.its].astype(F32)
        return value

    def hop(self, t, first, count, dr, dy):
        m, part = self.m, pl.ds(first, count)
        to = m.peer(m.offsets.index((dr, dy)))
        self.hops[t, first] = self.cp.push(self.tx.at[t, part, self.its], self.rg.at[t, part, self.its], to)

    def middle(self, t):
        m = self.m
        for j in range(1, m.tp):
            self.pair[t, j].wait_recv()
        for dr in range(1, m.R):
            for dy in range(2):
                self.tx[t, 2 * (dr - 1) + dy, self.its] = self.total(t, 0, dr, dy).astype(BF16)
            self.hop(t, 2 * (dr - 1), 2, dr, 0)
        for dr in range(m.R):
            self.tx[t, self.side + dr, self.its] = self.total(t, 1, dr, 1).astype(BF16)
        self.hop(t, self.side, m.R, 0, 1)
        for e in range(2):
            self.acc[self.place(t), e, self.its] = self.total(t, e, 0, 0)

    def relay(self, t):
        m = self.m

        def got(slot):
            return self.rg[t, slot, self.its].astype(F32)

        mine, other = self.acc[self.place(t), 0, self.its], self.total(t, 0, 0, 1)
        for dr in range(1, m.R):
            self.hops[t, 2 * (dr - 1)].wait_recv()
            mine, other = mine + got(2 * (dr - 1)), other + got(2 * (dr - 1) + 1)
        self.tx[t, self.cross, self.its] = other.astype(BF16)
        self.hop(t, self.cross, 1, 0, 1)
        self.acc[self.place(t), 0, self.its] = mine
        self.hops[t, self.side].wait_recv()
        for dr in range(1, m.R):
            value = self.total(t, 1, dr, 0) + got(self.side + dr)
            self.tx[t, self.back + dr - 1, self.its] = value.astype(BF16)
            self.hop(t, self.back + dr - 1, 1, dr, 0)
        self.acc[self.place(t), 1, self.its] += got(self.side)

    def end(self, t):
        m = self.m
        self.hops[t, self.cross].wait_recv()
        self.acc[self.place(t), 0, self.its] += self.rg[t, self.cross, self.its].astype(F32)
        for dr in range(1, m.R):
            self.hops[t, self.back + dr - 1].wait_recv()
            self.acc[self.place(t), 1, self.its] += self.rg[t, self.back + dr - 1, self.its].astype(F32)

    def finish(self):
        for copy in list(self.pair.values()) + list(self.hops.values()):
            copy.wait_send()


def flat(v):
    return v.reshape(-1, v.shape[-1])


def dot(a, b, ca, cb):
    return lax.dot_general(a, b, (((ca,), (cb,)), ((), ())), preferred_element_type=F32)


def unit_scale(v):
    return lax.rsqrt(jnp.mean(v * v, axis=-1, keepdims=True) + eps)


def kernel(sizes, D, nw, *refs):
    away, refs = refs[:nw], refs[nw:]
    ws, load, refs = refs[-nw - 1:-1], refs[-1], refs[:-nw - 1]
    loads = [pltpu.make_async_copy(away[i], ws[i], load.at[i]) for i in range(nw)]
    for copy in loads:
        copy.start()
    (x_late, x_early, cot, pre_gain, post_gain, y_out, dx_out, owned_out,
     wout, xout, dpost, gate, up, hid, hout, p, rx, tx, rg, acc, dall, dhid, dgate, dup, dz,
           q, qx, qt, qg, dacc, dw, sems) = refs
    m = Grid(sizes)
    cp = Copies(sems)
    n, fy, tp, fz = len(m.offsets), m.fy, m.tp, m.fz
    m.barrier(group=True, pair=True, levels=True)
    for copy in loads:
        copy.wait()
    f = m.z * fy + m.y
    rows, part = x_late.shape[0], wout.shape[-1]
    ce, drows = rows // tp, D // m.fs

    def weight(g, i):
        if nw == 1:
            return ws[0].at[g, i]
        return ws[i].at[:, pl.ds(pl.multiple_of(g * part, part), part)]

    def owned_at(g):
        if nw == 1:
            return owned_out.at[g]
        return owned_out.at[:, pl.ds(pl.multiple_of(g * part, part), part)]

    def columns(block):
        return slice(block * drows, (block + 1) * drows)

    def where(z, c):
        e, i = c
        return wout.at[i, z * fy + lax.rem(m.y + e, fy)]

    def first(c):
        return weight(m.g, c[1]) if c[0] == 0 else where(m.z, c)

    ys = {}

    def trade(i):
        for e in range(1, fy):
            o = m.offsets.index((0, e))
            ys[e, i] = cp.push(weight(m.index(o), i), wout.at[i, f], m.peer(o))

    ring_a = Ring(m, cp, first, where, [(e, i) for i in (0, 1) for e in range(fy)])
    ring_b = Ring(m, cp, first, where, [(e, 2) for e in range(fy)])
    trade(0)
    trade(1)
    for i in (0, 1):
        ring_a.send(0, 1, (0, i))
        ring_a.send(1, 1, (0, 1 - i))
    for t in range(tp):
        for place, ref in ((0, x_late), (ce, x_early)):
            v = ref[t * ce:(t + 1) * ce].astype(F32)
            v = (v * unit_scale(v) * pre_gain[...]).astype(BF16)
            for block in range(m.fs):
                xout[m.g, t, block, place:place + ce] = v[:, columns(block)]
    for i in range(3):
        wout[i, f] = weight(m.g, i)[...]
    xs = {o: cp.push(xout.at[m.g, m.k], xout.at[m.g, m.k], m.peer(o)) for o in range(n)}
    trade(2)
    mine = pl.ds(pl.multiple_of(m.k * ce, ce), ce)
    v = 0.5 * cot[mine].astype(F32) * post_gain[...]
    for block in range(m.fs):
        dpost[block] = v[:, columns(block)]
    for e in range(1, fy):
        back = (fy - e) % fy
        for i in (0, 1):
            ys[back, i].wait_recv()
        for i in (0, 1):
            ring_a.send(0, 1, (e, i))
            ring_a.send(1, 1, (e, 1 - i))
    for i in (0, 1):
        ring_a.arrive(0, 1, (0, i))
        ring_a.arrive(1, 1, (0, 1 - i))
    passed = []

    def spread(copies, out):
        for o in copies:
            copies[o].wait_recv()
            src = m.index(o, -1)
            for j in range(1, tp):
                passed.append(cp.push(out.at[src, m.k], out.at[src, m.k], m.sibling(j)))

    spread(xs, xout)
    ring_a.step(1)
    for d in (0, 1):
        ring_b.send(d, 1, (0, 2))
    for copy in passed:
        copy.wait()
    passed.clear()

    gate[...] = jnp.zeros_like(gate)
    up[...] = jnp.zeros_like(up)
    for dist, s, ds in stages(m):
        for d in ds:
            ring_a.step(s, (d,))
        if s == m.fz // 2:
            for e in range(1, fy):
                ys[(fy - e) % fy, 2].wait_recv()
                for d in (0, 1):
                    ring_b.send(d, 1, (e, 2))
        zt = m.along(dist)
        for e in range(fy):
            block = zt * fy + e

            def add(i, carry, block=block):
                rows = flat(xout[i, :, block])
                gate[i] += dot(rows, wout[0, block], 1, 0)
                up[i] += dot(rows, wout[1, block], 1, 0)
                return carry

            lax.fori_loop(0, m.G, add, 0)

    def activate(i, carry):
        v = gate[i]
        hid[i] = (v * (1.0 / (1.0 + jnp.exp(-v))) * up[i]).astype(BF16)
        return carry

    lax.fori_loop(0, m.G, activate, 0)
    for t in range(tp):
        hout[m.z, t] = hid[:, (2 * t + 1) * ce:(2 * t + 2) * ce]
    ring_h = Ring(m, cp, lambda c: hout.at[m.z, c], lambda z, c: hout.at[z, c], list(range(tp)))

    order = stages(m)
    halves = [pl.ds(low, ce) for low in (ce, 0)]
    sc, sl = (Scatter(m, cp, p, rx, tx, rg, acc, lambda t: m.along(order[t][0]), its) for its in halves)
    for t, (dist, s, ds) in enumerate(order):
        for d in ds:
            ring_b.step(s, (d,))
        if t == len(order) - 1:
            for i in range(tp):
                for d in (0, 1):
                    ring_h.send(d, 1, ring_h.order[d][i])
        zt = m.along(dist)
        for e in range(fy):
            block = zt * fy + e

            def product(i, carry, block=block, e=e):
                p[t, e, i] = dot(hid[i], wout[2, block], 1, 1).astype(BF16).reshape(p.shape[3:])
                return carry

            lax.fori_loop(0, m.G, product, 0)
        sc.start(t)
        sl.start(t)
        if t:
            sc.middle(t - 1)
        if t > 1:
            sc.relay(t - 2)
    sc.middle(len(order) - 1)
    sc.relay(len(order) - 2)
    sc.relay(len(order) - 1)
    for t in range(len(order)):
        sc.end(t)
    places = [divmod(block, fy) for block in range(m.fs)]

    def row_sum(term):
        return sum(jnp.sum(term(*place), axis=-1, keepdims=True) for place in places)

    rz = lax.rsqrt(row_sum(lambda t, e: acc[t, e, ce:] * acc[t, e, ce:]) / D + eps)
    mix = row_sum(lambda t, e: acc[t, e, ce:] * dpost[t * fy + e]) / D
    factor = rz * rz * mix
    for t, e in places:
        dall[m.g, m.k, t * fy + e] = (rz * (dpost[t * fy + e] - acc[t, e, ce:] * factor)).astype(BF16)
    dg = {o: cp.push(dall.at[m.g, m.k], dall.at[m.g, m.k], m.peer(o)) for o in range(n)}
    own = [cp.push(dall.at[m.g, m.k], dall.at[m.g, m.k], m.sibling(j)) for j in range(1, tp)]
    ring_h.step(1)
    for t in range(len(order)):
        sl.middle(t)
    spread(dg, dall)
    across = {}
    for s in range(1, fz):
        src = dall.at[:, m.k, pl.ds(m.along(s) * fy, fy)]
        across[s] = cp.push(src, dz.at[m.z, m.k], m.level(s))
    for copy in passed + own:
        copy.wait()
    passed.clear()

    def back(i, carry):
        total = dot(flat(dall[i, :, 0]), wout[2, 0], 1, 0)
        for block in range(1, m.fs):
            total = total + dot(flat(dall[i, :, block]), wout[2, block], 1, 0)
        dhid[i] = total
        return carry

    lax.fori_loop(0, m.G, back, 0)

    def gates(i, carry):
        for t in range(tp):
            its, to = pl.ds((2 * t + 1) * ce, ce), pl.ds(t * ce, ce)
            g, dh = gate[i, its], dhid[i, to]
            sig = 1.0 / (1.0 + jnp.exp(-g))
            dgate[i, to] = (dh * up[i, its] * sig * (1.0 + g * (1.0 - sig))).astype(BF16)
            dup[i, to] = (dh * g * sig).astype(BF16)
        return carry

    lax.fori_loop(0, m.G, gates, 0)
    for t in range(len(order)):
        sl.relay(t)
    dsc = Scatter(m, cp, q, qx, qt, qg, dacc, lambda t: t)
    for t in range(fz):
        for e in range(fy):
            block = t * fy + e

            def terms(i, carry, block=block, e=e, t=t):
                v = dot(dgate[i], wout[0, block], 1, 1) + dot(dup[i], wout[1, block], 1, 1)
                q[t, e, i] = v.astype(BF16).reshape(q.shape[3:])
                return carry

            lax.fori_loop(0, m.G, terms, 0)
        dsc.start(t)
        if t:
            dsc.middle(t - 1)
        if t > 1:
            dsc.relay(t - 2)
    dsc.middle(fz - 1)
    dsc.relay(fz - 2)
    dsc.relay(fz - 1)
    for s in range(2, ring_h.half + 1):
        ring_h.step(s)
    dz[m.z] = jnp.stack([dall[:, t, pl.ds(m.z * fy, fy)] for t in range(tp)])
    for s in across:
        across[s].wait_recv()
        src = m.along(-s)
        for j in range(1, tp):
            passed.append(cp.push(dz.at[src, m.k], dz.at[src, m.k], m.sibling(j)))
    for copy in passed:
        copy.wait()
    sends = []

    def gradient(r, e):
        a = dz[:, :, pl.ds(r * fy, fy), e]
        b = hout[:, :, pl.ds(r * fy, fy)]
        return dot(flat(a), flat(b), 0, 0).astype(BF16)

    for o in reversed(range(n)):
        r, y = m.moved(o)
        dw[o] = gradient(r, y)
        sends.append(cp.push(dw.at[o], owned_at(m.g), m.peer(o)))
    owned_at(m.g)[...] = gradient(m.r, m.y)
    for t in range(len(order)):
        sl.end(t)
    late_rz = lax.rsqrt(row_sum(lambda t, e: acc[t, e, :ce] * acc[t, e, :ce]) / D + eps)
    for t, e in places:
        cols = columns(t * fy + e)
        v = 0.5 * acc[t, e, :ce] * late_rz * post_gain[:, cols]
        y_out[m.k, :, cols] = (x_late[mine, cols].astype(F32) + v).astype(BF16)
    late = [cp.push(y_out.at[m.k], y_out.at[m.k], m.sibling(j)) for j in range(1, tp)]
    for t in range(fz):
        dsc.end(t)
    xf = x_early[mine].astype(F32)
    rs = unit_scale(xf)
    gained = lambda t, e: dacc[t, e] * pre_gain[:, columns(t * fy + e)]
    mix = row_sum(lambda t, e: gained(t, e) * xf[:, columns(t * fy + e)]) / D
    factor = rs * rs * mix
    for t, e in places:
        cols = columns(t * fy + e)
        v = rs * (gained(t, e) - xf[:, cols] * factor)
        dx_out[m.k, :, cols] = (cot[mine, cols].astype(F32) + v).astype(BF16)
    last = [cp.push(dx_out.at[m.k], dx_out.at[m.k], m.sibling(j)) for j in range(1, tp)]
    for copy in sends + last + late:
        copy.wait()
    for copies in (xs, ys, dg, across):
        for copy in copies.values():
            copy.wait_send()
    for thing in (ring_a, ring_b, ring_h, sc, sl, dsc):
        thing.finish()


def body(sizes, x_late, x_early, cotangent, pre_gain, post_gain, gate_weight, up_weight, down_weight,
         down_grad_sum):
    R, fs, tp = sizes
    fy = 2
    fz, G = fs // fy, R * fy
    rows, D = x_late.shape
    drows, width = gate_weight.shape
    part = width // G
    n = G - 1
    ce = rows // tp
    c = 2 * ce
    S, V = jax.ShapeDtypeStruct, pltpu.VMEM

    weights = [gate_weight, up_weight, down_weight]
    aligned = part % 128 == 0
    if not aligned:
        weights = [jnp.stack([w.reshape(drows, G, part) for w in weights]).transpose(2, 0, 1, 3)]
    ring = 2 * (fz // 2)
    count = (3 * (fy - 1) + ring * (3 * fy + tp) + 2 * (n + n * (tp - 1)) + 3 * (tp - 1)
             + 3 * fz * (tp - 1 + 2 * R) + (fz - 1) * tp + n)

    def scatter(c):
        return [
            V((fz, fy, G, tp, c, drows), BF16),
            V((tp - 1, fz, fy, G, c, drows), BF16),
            V((fz, 4 * R - 2, c, drows), BF16),
            V((fz, 4 * R - 2, c, drows), BF16),
            V((fz, fy, c, drows), F32),
        ]

    all_rows, early_rows = tp * c, tp * ce
    y_late, dx_early, owned = pl.pallas_call(
        functools.partial(kernel, sizes, D, len(weights)),
        out_shape=[
            S((tp, ce, D), BF16), S((tp, ce, D), BF16),
            S((drows, width) if aligned else (G, drows, part), BF16),
        ],
        in_specs=[pl.BlockSpec(memory_space=pl.ANY)] * len(weights) + [VMEM] * 5,
        out_specs=[VMEM] * 3,
        scratch_shapes=[
            V((3, fs, drows, part), BF16),
            V((G, tp, fs, c, drows), BF16),
            V((fs, ce, drows), F32),
            V((G, all_rows, part), F32),
            V((G, all_rows, part), F32),
            V((G, all_rows, part), BF16),
            V((fz, tp, G, ce, part), BF16),
        ] + scatter(c) + [
            V((G, tp, fs, ce, drows), BF16),
            V((G, early_rows, part), F32),
            V((G, early_rows, part), BF16),
            V((G, early_rows, part), BF16),
            V((fz, tp, G, fy, ce, drows), BF16),
        ] + scatter(ce) + [
            V((n, drows, part), BF16),
            DMA((2, count)),
        ] + [V(w.shape, w.dtype) for w in weights] + [DMA((len(weights),))],
        compiler_params=pltpu.CompilerParams(
            collective_id=0, has_side_effects=True, vmem_limit_bytes=60 * 1024 * 1024
        ),
    )(*weights, x_late, x_early, cotangent, pre_gain.reshape(1, D), post_gain.reshape(1, D))
    if not aligned:
        owned = owned.transpose(1, 0, 2).reshape(drows, width)
    down_grad_out = down_grad_sum + owned.astype(F32)
    return (y_late.reshape(rows, D), dx_early.reshape(rows, D), down_grad_out)


def solution(mesh):
    sizes = tuple(mesh.shape[a] for a in ("rep", "fs", "tp"))
    in_specs = (
        P(("rep", "fs"), None),
        P(("rep", "fs"), None),
        P(("rep", "fs"), None),
        P(),
        P(),
        P("fs", "tp"),
        P("fs", "tp"),
        P("fs", "tp"),
        P(("rep", "fs"), "tp"),
    )
    out_specs = (P(("rep", "fs"), None), P(("rep", "fs"), None), P(("rep", "fs"), "tp"))
    return jax.shard_map(
        functools.partial(body, sizes), mesh=mesh, in_specs=in_specs, out_specs=out_specs, check_vma=False
    )
```
